256 devices in a mesh: ep: 64 (over z, x, core), tp: 4 (over y).
Axes of the slice: x: 4, y: 4, z: 8, core: 2. Of those that a mesh axis runs over, the one named last changes fastest.
Arguments:
- queries: bfloat16 [16384, 1024], P('ep', 'tp'), may hold values from -6 to 6
- keys: bfloat16 [16384, 256], P('ep', 'tp'), may hold values from -6 to 6
- values: bfloat16 [16384, 256], P('ep', 'tp'), may hold values from -6 to 6
- q_gain: float32 [64], replicated, may hold values from 1 to 6
- k_gain: float32 [64], replicated, may hold values from 1 to 6
- out_weight: bfloat16 [1024, 2048], P('tp'), may hold values from -0.1875 to 0.1875
- tokens: bfloat16 [8192, 2048], P(('ep', 'tp')), may hold values from -6 to 6
- ffn_gain: float32 [2048], replicated, may hold values from 0.1 to 1.9
- route: int32 [8192, 2], P(('ep', 'tp')), may hold values from 0 to 63, all different within a row; in each aligned block of 32 rows (0 to 31, 32 to 63, ...) at most 2 rows name the same one
- route_weight: float32 [8192, 2], P(('ep', 'tp')), may hold values from 0.1 to 1
- gate_weight: bfloat16 [64, 2048, 3584], P('ep', None, 'tp'), may hold values from -0.125 to 0.125
- up_weight: bfloat16 [64, 2048, 3584], P('ep', None, 'tp'), may hold values from -0.125 to 0.125
- down_weight: bfloat16 [64, 3584, 2048], P('ep', 'tp'), may hold values from -0.09375 to 0.09375
Outputs:
- mixer_out: bfloat16 [16384, 2048], P(('ep', 'tp'))
- mixed: bfloat16 [8192, 2048], P(('ep', 'tp'))
The draws below stay inside these ranges and needn't reach their ends.
Inputs may be any that keep to these rules, and one draw needn't show every extreme that they name: `route`: each row names 2 different experts. In every device's aligned block of 32 rows no expert is named more than 2 times, and in some blocks some expert is named exactly 2 times.
All inputs are finite; a program needn't handle non-finite values.
Results may differ from the reference program's by a relative error of at most 0.013.
The reference program's roundings to bfloat16 on the way count: a program that leaves them out, or rounds other values in their place, can miss the bound.
Values may be sent and summed in bfloat16 or wider, within the bound.
A program may use at most 192 MiB of HBM per device.

```python
import math
import jax
import jax.numpy as jnp
import numpy as np
from jax import lax

D = 2048
HEADS = 16
KV_HEADS = 4
HEAD_DIM = 64
FF = 3584
TOPK = 2
GRID_W = 64
TOKENS_A = 16384
TOKENS_B = 8192
EXPERTS = 64
ROUTE_ROWS = 32
CAPACITY = 2
QW = 1024
KVW = 256
N_TP = 4


def draw_gain(key, salt):
    inner = jax.random.fold_in(key, salt)
    logs = jax.random.uniform(inner, (HEAD_DIM,), jnp.float32, 0.0, math.log(2.5))
    return jnp.exp(logs)


def draw_q_gain(key, part):
    return draw_gain(key, 21)


def draw_k_gain(key, part):
    return draw_gain(key, 22)


def draw_pair(key):
    query_key = jax.random.fold_in(key, 41)
    key_key = jax.random.fold_in(key, 42)
    query_vals = jnp.clip(jax.random.normal(query_key, (TOKENS_A, HEADS, HEAD_DIM), jnp.float32), -6.0, 6.0)
    key_vals = jnp.clip(jax.random.normal(key_key, (TOKENS_A, KV_HEADS, HEAD_DIM), jnp.float32), -6.0, 6.0)
    return (query_vals.reshape(TOKENS_A, HEADS * HEAD_DIM), key_vals.reshape(TOKENS_A, KV_HEADS * HEAD_DIM))


def draw_queries(key, part):
    return draw_pair(key)[0].astype(jnp.bfloat16)


def draw_keys(key, part):
    return draw_pair(key)[1].astype(jnp.bfloat16)


def block_levels(own_key, extent, shards, smallest, top_value):
    loudness = 1.0
    for position, blocks in shards:
        heights = jax.random.uniform(jax.random.fold_in(jax.random.fold_in(own_key, 6), position), (blocks,), jnp.float32, smallest / len(shards), top_value / len(shards))
        loudness = loudness * jnp.repeat(jnp.exp(heights), extent[position] // blocks).reshape((-1,) + (1,) * (len(extent) - 1 - position))
    return loudness


def assign_block(stream_key, own, number, rows, amount, top, reach, skew):
    order = jax.random.permutation(stream_key, amount)
    crowded, usual = portions_of(amount, rows * top, reach, skew, True), portions_of(amount, rows * top, reach, skew, False)
    places = jnp.arange(amount)

    def named(sizes, turn):
        used = int((sizes > 0).sum())
        fixed = max(1, used // 4)
        passed = fixed + (places - fixed + turn * (used - fixed)) % max(1, amount - fixed)
        return jnp.zeros((amount,), jnp.int32).at[order[jnp.where(places < fixed, places, passed)]].set(jnp.asarray(sizes, jnp.int32))

    sizes = jnp.where(number % 4 == 0, named(crowded, number // 4), named(usual, number - number // 4 - 1))
    mixed = jax.random.permutation(jax.random.fold_in(own, 3), amount)
    source_of, sink = mixed[0:amount // 2 * 2:2], mixed[1:amount // 2 * 2:2]
    slack = jnp.minimum(sizes[source_of] - 1, reach - sizes[sink]) // 2
    slack = jnp.where((source_of == order[0]) | (sink == order[0]) | (sizes[sink] == 0), 0, jnp.maximum(slack, 0))
    passed = jax.random.randint(jax.random.fold_in(own, 4), (amount // 2,), 0, 1 << 20) % (slack + 1)
    sizes = sizes.at[source_of].add(-passed).at[sink].add(passed)
    items = jnp.searchsorted(jnp.cumsum(sizes), jnp.arange(rows * top), side="right").astype(jnp.int32)
    grid = items.reshape(top, rows).T
    grid = grid[jax.random.permutation(jax.random.fold_in(own, 1), rows)]
    turn = jax.random.randint(jax.random.fold_in(own, 2), (rows, 1), 0, top)
    return jnp.take_along_axis(grid, (jnp.arange(top)[None, :] + turn) % top, axis=1)


def portions_of(number_of, total, reach, slope, full):
    portions = [(1 << 20) // math.isqrt(rank ** slope) + 1 for rank in range(1, number_of + 1)]
    largest = reach if full else min(reach, max(-(-total // number_of), total * portions[0] // sum(portions)))
    least = 1 if total - largest >= number_of - 1 else 0
    counts, surplus = [largest] + [least] * (number_of - 1), total - largest - least * (number_of - 1)
    while surplus > 0:
        movable = [i for i in range(1, number_of) if counts[i] < largest] or [i for i in range(1, number_of) if counts[i] < reach]
        mass, remaining = sum([portions[i] for i in movable]), surplus
        for i in movable:
            addition = min(reach - counts[i], max(1, remaining * portions[i] // mass), surplus)
            counts[i] = counts[i] + addition
            surplus = surplus - addition
    return np.array(counts)


def normal_values(own_key, extent, scale, most, cuts=(), kind=jnp.bfloat16):
    entries = scale * jax.random.normal(own_key, extent, jnp.float32)
    if cuts:
        entries = entries * block_levels(own_key, extent, cuts, -0.22, 0.18)
    return jnp.clip(entries, -most, most).astype(kind)


def setup_inputs(seed: int = 0) -> dict:
    splits = jax.random.split(jax.random.key(seed), 14)
    queries = draw_queries(jax.random.fold_in(splits[13], 71), 0)
    keys = draw_keys(jax.random.fold_in(splits[13], 71), 0)
    values = normal_values(splits[2], (TOKENS_A, KVW), 1.0, 6.0, ((0, 64), (1, 4)))
    q_gain = draw_q_gain(jax.random.fold_in(splits[13], 71), 0)
    k_gain = draw_k_gain(jax.random.fold_in(splits[13], 71), 0)
    out_weight = normal_values(splits[5], (QW, D), QW ** -0.5, 0.1875, ((0, 4),))
    tokens = normal_values(splits[6], (TOKENS_B, D), 1.0, 6.0, ((0, 256),))
    ffn_gain = jnp.clip(1.0 + 0.18 * jax.random.normal(splits[7], (D,), jnp.float32), 0.1, 1.9)
    route_keys = jax.random.split(jax.random.fold_in(splits[8], 1), TOKENS_B // ROUTE_ROWS)
    route_turns = jax.random.permutation(jax.random.fold_in(splits[8], 3), TOKENS_B // ROUTE_ROWS)
    route = jax.vmap(lambda own, number: assign_block(jax.random.fold_in(splits[8], 2), own, number, ROUTE_ROWS, EXPERTS, TOPK, CAPACITY, 1))(route_keys, route_turns).reshape((TOKENS_B, TOPK))
    route_weight = jnp.clip(0.1 + 0.9 * jax.random.uniform(splits[9], (TOKENS_B, TOPK), jnp.float32) ** block_levels(splits[9], (TOKENS_B, TOPK), ((0, 256),), -0.2, 0.2), 0.1, 1.0)
    gate_weight = normal_values(splits[10], (EXPERTS, D, FF), D ** -0.5, 0.125, ((0, 64), (2, 4)))
    up_weight = normal_values(splits[11], (EXPERTS, D, FF), D ** -0.5, 0.125, ((0, 64), (2, 4)))
    down_weight = normal_values(splits[12], (EXPERTS, FF, D), FF ** -0.5, 0.09375, ((0, 64), (1, 4)))
    return dict(queries=queries, keys=keys, values=values, q_gain=q_gain, k_gain=k_gain, out_weight=out_weight, tokens=tokens, ffn_gain=ffn_gain, route=route, route_weight=route_weight, gate_weight=gate_weight, up_weight=up_weight, down_weight=down_weight)


EPS = 1e-06
THETA = 10000.0

def head_norm(vals, gain):
    vals = vals.astype(jnp.float32)
    return vals * lax.rsqrt(lax.optimization_barrier(jnp.mean(vals * vals, axis=-1, keepdims=True)) + EPS) * gain

def rotate(vals, positions):
    pairs = vals.shape[-1] // 2
    quarter = pairs // 2
    freqs = THETA ** (-jnp.arange(quarter, dtype=jnp.float32) / quarter)
    grid_row = (positions // GRID_W).astype(jnp.float32)
    grid_col = (positions % GRID_W).astype(jnp.float32)
    angle = jnp.concatenate([grid_row[:, None] * freqs, grid_col[:, None] * freqs], axis=-1)
    cosine = jnp.cos(angle)[:, None, :]
    sine = jnp.sin(angle)[:, None, :]
    split = vals.reshape(vals.shape[:-1] + (pairs, 2))
    first = split[..., 0]
    second = split[..., 1]
    turned = jnp.stack([first * cosine - second * sine, first * sine + second * cosine], axis=-1)
    return turned.reshape(vals.shape)

def reference(queries, keys, values, q_gain, k_gain, out_weight, tokens, ffn_gain, route, route_weight, gate_weight, up_weight, down_weight):
    total = queries.shape[0]
    group = HEADS // KV_HEADS
    positions = jnp.arange(total, dtype=jnp.int32)
    rot_q = rotate(head_norm(queries.reshape(total, HEADS, HEAD_DIM), q_gain), positions).astype(jnp.bfloat16)
    rot_k = rotate(head_norm(keys.reshape(total, KV_HEADS, HEAD_DIM), k_gain), positions).astype(jnp.bfloat16)
    key_float = rot_k.astype(jnp.float32)
    value_float = values.reshape(total, KV_HEADS, HEAD_DIM).astype(jnp.float32)
    scale = HEAD_DIM ** (-0.5)
    block = math.gcd(total, 256)

    def attend(query_block):
        scores = jnp.einsum('qkgd,skd->qkgs', query_block.astype(jnp.float32), key_float) * scale
        highest = lax.optimization_barrier(jnp.max(scores, axis=-1, keepdims=True))
        expo = jnp.exp(scores - highest)
        denom = lax.optimization_barrier(jnp.sum(expo, axis=-1))
        probs = lax.optimization_barrier(expo.astype(jnp.bfloat16)).astype(jnp.float32)
        numer = jnp.einsum('qkgs,skd->qkgd', probs, value_float)
        return (numer / denom[..., None]).astype(jnp.bfloat16)
    query_blocks = rot_q.reshape(total // block, block, KV_HEADS, group, HEAD_DIM)
    attended = lax.map(attend, query_blocks).reshape(total, QW)
    share = QW // N_TP
    summed = jnp.zeros((total, D), jnp.float32)
    for index in range(N_TP):
        part = jnp.dot(attended[:, index * share:(index + 1) * share], out_weight[index * share:(index + 1) * share], preferred_element_type=jnp.float32)
        summed = summed + part.astype(jnp.bfloat16).astype(jnp.float32)
    mixer_out = summed.astype(jnp.bfloat16)
    token_float = tokens.astype(jnp.float32)
    normed = (token_float * lax.rsqrt(lax.optimization_barrier(jnp.mean(token_float * token_float, axis=-1, keepdims=True)) + EPS) * ffn_gain).astype(jnp.bfloat16)
    picks = route.reshape(-1)
    count = picks.shape[0]
    limit = tokens.shape[0] // ROUTE_ROWS * CAPACITY
    hidden_share = FF // N_TP

    def one_expert(expert):
        order = jnp.argsort((picks != expert).astype(jnp.int32), stable=True)[:limit].astype(jnp.int32)
        valid = picks[order] == expert
        chosen = normed[order // TOPK]
        gate = jnp.dot(chosen, gate_weight[expert], preferred_element_type=jnp.float32)
        upper = jnp.dot(chosen, up_weight[expert], preferred_element_type=jnp.float32)
        hidden = (jax.nn.silu(gate) * upper).astype(jnp.bfloat16)
        down = down_weight[expert]
        result = jnp.zeros((limit, D), jnp.float32)
        for index in range(N_TP):
            part = jnp.dot(hidden[:, index * hidden_share:(index + 1) * hidden_share], down[index * hidden_share:(index + 1) * hidden_share], preferred_element_type=jnp.float32)
            result = result + part.astype(jnp.bfloat16).astype(jnp.float32)
        target = jnp.where(valid, order, count).astype(jnp.int32)
        return (result.astype(jnp.bfloat16), target)
    outputs, targets = lax.map(one_expert, jnp.arange(EXPERTS, dtype=jnp.int32))
    per_pick = jnp.zeros((count, D), jnp.bfloat16).at[targets.reshape(-1)].set(outputs.reshape(-1, D), mode='drop')
    weighted = route_weight[..., None] * per_pick.reshape(tokens.shape[0], TOPK, D).astype(jnp.float32)
    mixed = lax.optimization_barrier(jnp.sum(weighted, axis=1)).astype(jnp.bfloat16)
    return (mixer_out, mixed)
```

```python
import functools

import jax
import jax.numpy as jnp
from jax import lax
from jax.experimental import pallas as pl
from jax.experimental.pallas import tpu as pltpu
from jax.sharding import PartitionSpec as P

GRID_W = 64
EPS = 1e-06
THETA = 10000.0

NZ, NX = 8, 4
PLANES = (0, 7, 1, 6, 2, 5, 3, 4)
BF = jnp.bfloat16
F32 = jnp.float32
MESH = pl.DeviceIdType.MESH
RIGHT, OPP, LEFT = 1, 2, 3
F0, F1, D0, D1, E0, E1, S0, S1 = range(8)


def head_norm(vals, gain):
    vals = vals.astype(F32)
    return vals * lax.rsqrt(jnp.mean(vals * vals, axis=-1, keepdims=True) + EPS) * gain


def rotate(vals, positions):
    pairs = vals.shape[-1] // 2
    quarter = pairs // 2
    freqs = THETA ** (-jnp.arange(quarter, dtype=F32) / quarter)
    grid_row = (positions // GRID_W).astype(F32)
    grid_col = (positions % GRID_W).astype(F32)
    angle = jnp.concatenate([grid_row[:, None] * freqs, grid_col[:, None] * freqs], axis=-1)
    cosine = jnp.cos(angle)[:, None, :]
    sine = jnp.sin(angle)[:, None, :]
    split = vals.reshape(vals.shape[:-1] + (pairs, 2))
    first = split[..., 0]
    second = split[..., 1]
    turned = jnp.stack([first * cosine - second * sine, first * sine + second * cosine], axis=-1)
    return turned.reshape(vals.shape)


def body(
    q_ref,
    kvin_ref,
    outg_ref,
    gate_hbm,
    up_hbm,
    down_hbm,
    ow_hbm,
    mix_ref,
    back_ref,
    kv,
    xs,
    xm,
    hid,
    part,
    rsb,
    ret,
    att,
    m_s,
    acc,
    gate_v,
    up_v,
    down_v,
    ow_v,
    ssem,
    rsem,
    lsem,
):
    e = lax.axis_index("ep")
    t = lax.axis_index("tp")
    z, x, c = e // 8, lax.rem(e // 2, NX), lax.rem(e, 2)

    def dev(dz, dx, dc, dt=0):
        zz = lax.rem(z + (dz + NZ), NZ)
        xx = lax.rem(x + (dx + NX), NX)
        cc = c if dc == 0 else 1 - c
        tt = t if dt == 0 else lax.rem(t + (dt + 4), 4)
        return (zz * 8 + xx * 2 + cc, tt)

    used = [0]

    def sems():
        used[0] += 1
        return used[0] - 1

    def copy(src, dst, device, i=None):
        i = sems() if i is None else i
        return pltpu.make_async_remote_copy(
            src_ref=src,
            dst_ref=dst,
            send_sem=ssem.at[i],
            recv_sem=rsem.at[i],
            device_id=device,
            device_id_type=MESH,
        )

    kx = {
        3: copy(kvin_ref, kv.at[0, 0, 3], dev(0, 1, 0)),
        1: copy(kvin_ref, kv.at[0, 0, 1], dev(0, -1, 0)),
        2: copy(kvin_ref, kv.at[0, 0, 2], dev(0, 2, 0)),
    }
    kp0 = copy(kvin_ref, kv.at[0, 1, 0], dev(0, 0, 1))
    kpx = copy(kv.at[0, 0, pl.ds(1, 3)], kv.at[0, 1, pl.ds(1, 3)], dev(0, 0, 1))
    up_dev, down_dev, partner = dev(1, 0, 0), dev(-1, 0, 0), dev(0, 0, 1)
    hop_up = [copy(kv.at[(8 - i) % 8, 0], kv.at[7 - i, 0], up_dev) for i in range(3)]
    hop_down = [copy(kv.at[i, 0], kv.at[i + 1, 0], down_dev) for i in range(3)]
    hop_up.append(copy(kv.at[5, 0, pl.ds(0, 2)], kv.at[4, 0, pl.ds(0, 2)], up_dev))
    hop_down.append(copy(kv.at[3, 0, pl.ds(2, 2)], kv.at[4, 0, pl.ds(2, 2)], down_dev))
    pz = {d: copy(kv.at[d, 0], kv.at[d, 1], partner) for d in range(1, NZ)}

    spots = [
        (p, dx, dc) for p in range(NZ) for dx in range(NX) for dc in range(2)
    ]
    dsp_i, ret_i = [sems(), sems()], [sems(), sems()]
    dispatch, returns = [[], []], [[], []]
    for k, (p, dx, dc) in enumerate(spots):
        if k == 0:
            continue
        ch, j = k // 32, k % 32
        dz = PLANES[p]
        dispatch[ch].append(copy(outg_ref.at[k], xs.at[ch, 0, j], dev(-dz, -dx, dc), dsp_i[ch]))
        returns[ch].append(copy(ret.at[ch, j], back_ref.at[k], dev(dz, dx, dc), ret_i[ch]))

    def span(ref, ch):
        return ref.at[pl.ds(1, 31)] if ch == 0 else ref.at[pl.ds(0, 32)]

    def dispatch_all(ch):
        view = span(xs.at[ch, 0], ch)
        return copy(view, view, partner, dsp_i[ch])

    def return_all(ch):
        view = back_ref.at[pl.ds(1, 31)] if ch == 0 else back_ref.at[pl.ds(32, 32)]
        return copy(view, view, partner, ret_i[ch])

    right, left = dev(0, 0, 0, 1), dev(0, 0, 0, -1)
    lo, hi = pl.ds(0, 16), pl.ds(16, 16)
    ag = []
    for ch in range(2):
        ag.append(
            (
                copy(xs.at[ch, 0, lo], xs.at[ch, LEFT, lo], right),
                copy(xs.at[ch, 0, hi], xs.at[ch, RIGHT, hi], left),
                copy(xs.at[ch, 0, hi], xs.at[ch, LEFT, hi], right),
                copy(xs.at[ch, 0, lo], xs.at[ch, RIGHT, lo], left),
                copy(xs.at[ch, LEFT, lo], xs.at[ch, OPP, lo], right),
                copy(xs.at[ch, RIGHT, hi], xs.at[ch, OPP, hi], left),
            )
        )
    lo, hi = pl.ds(0, 32), pl.ds(32, 32)
    rs = []
    for i in range(3):
        pi, bi = part.at[i], rsb.at[i]
        rs.append(
            (
                copy(pi.at[OPP, lo], bi.at[F0], right),
                copy(pi.at[OPP, hi], bi.at[F1], left),
                copy(pi.at[RIGHT, hi], bi.at[D1], right),
                copy(pi.at[LEFT, lo], bi.at[D0], left),
                copy(bi.at[S0], bi.at[E0], right),
                copy(bi.at[S1], bi.at[E1], left),
            )
        )

    loads = [
        pltpu.make_async_copy(src, dst, lsem.at[i])
        for i, (src, dst) in enumerate(
            [(gate_hbm, gate_v), (up_hbm, up_v), (down_hbm, down_v), (ow_hbm, ow_v)]
        )
    ]

    def gather_first(ch):
        dispatch_all(ch).wait_recv()
        for one in ag[ch][:4]:
            one.start()

    def gather_second(ch):
        ag[ch][0].wait_recv()
        ag[ch][4].start()
        ag[ch][1].wait_recv()
        ag[ch][5].start()

    def reduce_first(i):
        for one in rs[i][:4]:
            one.start()

    def reduce_second(i):
        for copied, slot, other, half, sent, way in (
            (0, F0, RIGHT, 0, S0, 4),
            (1, F1, LEFT, 32, S1, 5),
        ):
            rs[i][copied].wait_recv()
            for r in range(2):
                rows = pl.ds(16 * r, 16)
                own = part[i, other, pl.ds(half + 16 * r, 16)].astype(F32)
                rsb[i, sent, rows] = (rsb[i, slot, rows].astype(F32) + own).astype(BF)
            rs[i][way].start()

    def reduce_last(i, store):
        for direct, passed, d, pe, half in ((3, 4, D0, E0, 0), (2, 5, D1, E1, 32)):
            rs[i][direct].wait_recv()
            rs[i][passed].wait_recv()
            for r in range(2):
                rows = pl.ds(16 * r, 16)
                total = (
                    part[i, 0, pl.ds(half + 16 * r, 16)].astype(F32)
                    + rsb[i, d, rows].astype(F32)
                    + rsb[i, pe, rows].astype(F32)
                ).astype(BF)
                store(half + 16 * r, total)

    def experts(ch):
        for n in (2, 3, 4, 5):
            ag[ch][n].wait_recv()
        if ch == 0:
            for one in loads[:3]:
                one.wait()

        def relay(g, _):
            r, q = g // 4, lax.rem(g, 4)
            rows = xs[ch, r, pl.ds(q * 8, 8)].reshape(16, 2048)
            xm[pl.ds(pl.multiple_of(g * 16, 16), 16), :] = rows
            return 0

        lax.fori_loop(0, 16, relay, 0)

        def widen(n, _):
            cols = pl.ds(pl.multiple_of(n * 128, 128), 128)
            both = jnp.concatenate([gate_v[:, cols], up_v[:, cols]], axis=1)
            made = jnp.dot(xm[...], both, preferred_element_type=F32)
            gate, upper = made[:, :128], made[:, 128:]
            hid[:, cols] = (gate / (1.0 + jnp.exp(-gate)) * upper).astype(BF)
            return 0

        lax.fori_loop(0, 7, widen, 0)

        def narrow(n, _):
            cols = pl.ds(pl.multiple_of(n * 256, 256), 256)
            made = jnp.dot(hid[...], down_v[:, cols], preferred_element_type=F32).astype(BF)
            for r in range(4):
                part[ch, r, :, cols] = made[r * 64 : (r + 1) * 64]
            return 0

        lax.fori_loop(0, 8, narrow, 0)
        reduce_first(ch)

    def give_back(ch):
        def store(row, total):
            ret[ch, pl.ds(row // 2, 8)] = total.reshape(8, 2, 2048)

        reduce_last(ch, store)
        if ch == 0:
            back_ref[0] = ret[0, 0]
        for one in returns[ch]:
            one.start()

    barrier = pltpu.get_barrier_semaphore()
    for k, (p, dx, dc) in enumerate(spots):
        if k:
            pl.semaphore_signal(
                barrier, inc=1, device_id=dev(PLANES[p], dx, dc), device_id_type=MESH
            )
    for peer in (right, left):
        pl.semaphore_signal(barrier, inc=1, device_id=peer, device_id_type=MESH)
    for one in loads:
        one.start()
    kv[0, 0, 0] = kvin_ref[...]
    xs[0, 0, 0] = outg_ref[0]
    m_s[...] = jnp.full_like(m_s, -1e30)
    acc[...] = jnp.zeros_like(acc)
    pl.semaphore_wait(barrier, 65)

    kp0.start()
    for one in kx.values():
        one.start()
    for ch in range(2):
        for one in dispatch[ch]:
            one.start()
    for one in kx.values():
        one.wait_recv()
    kpx.start()
    hop_up[0].start()
    hop_down[0].start()
    gather_first(0)
    kp0.wait_recv()
    kpx.wait_recv()

    def pass_on(i):
        hop_up[i].wait_recv()
        hop_down[i].wait_recv()
        if i < 3:
            hop_up[i + 1].start()
            hop_down[i + 1].start()
            pz[7 - i].start()
            pz[i + 1].start()
        else:
            pz[4].start()

    def at1():
        gather_second(0)
        gather_first(1)
        experts(0)
        gather_second(1)
        pass_on(0)
        pz[7].wait_recv()

    def at2():
        reduce_second(0)
        pz[1].wait_recv()

    def at3():
        experts(1)
        pass_on(1)
        give_back(0)
        pz[6].wait_recv()

    def at4():
        reduce_second(1)
        pz[2].wait_recv()

    def at5():
        pass_on(2)
        give_back(1)
        pz[5].wait_recv()

    def at6():
        pz[3].wait_recv()

    def at7():
        pass_on(3)
        pz[4].wait_recv()

    events = {1: at1, 2: at2, 3: at3, 4: at4, 5: at5, 6: at6, 7: at7}

    def step(s, _):
        for at, event in events.items():
            pl.when(s == at)(event)
        odd = lax.rem(s, 2)
        dz = odd * (8 - (s + 1) // 2) + (1 - odd) * (s // 2)
        keyed = kv[dz].reshape(2048, 128)
        lane = lax.broadcasted_iota(jnp.int32, keyed.shape, 1)
        valued = jnp.where(lane == 0, jnp.ones_like(keyed), keyed)

        def score(h):
            return lax.dot_general(
                q_ref[pl.ds(h * 256, 256), :],
                keyed,
                (((1,), (1,)), ((), ())),
                preferred_element_type=F32,
            )

        highs = [m_s[h] for h in range(4)]
        sums = [acc[h] for h in range(4)]
        new_high, new_sum = [], []
        ahead = score(0)
        for h in range(4):
            now = ahead
            if h < 3:
                ahead = score(h + 1)
            high = jnp.maximum(highs[h], jnp.max(now, axis=1, keepdims=True))
            probs = jnp.exp(now - high).astype(BF)
            made = jnp.dot(probs, valued, preferred_element_type=F32)
            new_sum.append(sums[h] * jnp.exp(highs[h] - high) + made)
            new_high.append(high)
        for h in range(4):
            m_s[h] = new_high[h]
            acc[h] = new_sum[h]
        return 0

    lax.fori_loop(0, 8, step, 0)

    for pair in range(2):
        both = []
        for h in (2 * pair, 2 * pair + 1):
            total = acc[h]
            both.append((total / total[:, 0:1])[:, 64:].astype(BF))
        att[:, pair * 128 : (pair + 1) * 128] = jnp.concatenate(both, axis=1)
    loads[3].wait()

    def project(n, _):
        cols = pl.ds(pl.multiple_of(n * 256, 256), 256)
        made = jnp.dot(att[...], ow_v[:, cols], preferred_element_type=F32).astype(BF)
        for b in range(4):
            part[2, lax.rem(b + 4 - t, 4), :, cols] = made[b * 64 : (b + 1) * 64]
        return 0

    lax.fori_loop(0, 8, project, 0)
    reduce_first(2)
    reduce_second(2)

    def store_mix(row, total):
        mix_ref[pl.ds(row, 16), :] = total

    reduce_last(2, store_mix)
    for ch in range(2):
        return_all(ch).wait_recv()
    for one in [*kx.values(), kp0, kpx, *hop_up, *hop_down, *pz.values()]:
        one.wait_send()
    for ch in range(2):
        dispatch_all(ch).wait_send()
        return_all(ch).wait_send()
        for one in ag[ch]:
            one.wait_send()
    for i in range(3):
        for one in rs[i]:
            one.wait_send()


def local(
    queries,
    keys,
    values,
    q_gain,
    k_gain,
    out_weight,
    tokens,
    ffn_gain,
    route,
    route_weight,
    gate_weight,
    up_weight,
    down_weight,
):
    e = lax.axis_index("ep")
    z, x, c = e // 8, (e // 2) % 4, e % 2
    positions = e * 256 + jnp.arange(256, dtype=jnp.int32)
    rot_q = rotate(head_norm(queries.reshape(256, 4, 64), q_gain), positions).astype(BF)
    rot_q = rot_q * jnp.asarray(0.125, BF)
    rot_q = jnp.pad(jnp.moveaxis(rot_q, 1, 0), ((0, 0), (0, 0), (0, 64))).reshape(1024, 128)
    rot_k = rotate(head_norm(keys.reshape(256, 1, 64), k_gain), positions).astype(BF)
    joined = jnp.concatenate([rot_k.reshape(256, 64), values], axis=1)

    token_float = tokens.astype(F32)
    normed = (
        token_float
        * lax.rsqrt(jnp.mean(token_float * token_float, axis=-1, keepdims=True) + EPS)
        * ffn_gain
    ).astype(BF)
    spot = jnp.arange(64, dtype=jnp.int32)
    place = spot // 8
    dz = jnp.where(place % 2 == 1, 8 - (place + 1) // 2, place // 2)
    dx, dc = (spot // 2) % 4, spot % 2
    target = ((z - dz) % 8) * 8 + ((x - dx) % 4) * 2 + (c + dc) % 2
    flat_route = route.reshape(-1)
    hot = (flat_route[:, None] == target[None, :]).astype(BF)
    before = (jnp.arange(64)[:, None] > jnp.arange(64)[None, :]).astype(BF)
    earlier = jnp.dot(before, hot, preferred_element_type=F32)
    rank = jnp.sum(earlier * hot.astype(F32), axis=1)
    ranked = (rank[:, None] == jnp.arange(2, dtype=F32)[None, :]).astype(BF)
    pick_hot = (hot[:, :, None] * ranked[:, None, :]).reshape(64, 128)
    row_hot = jnp.sum(pick_hot.reshape(32, 2, 128), axis=1)
    outgoing = jnp.einsum("rs,rd->sd", row_hot, normed, preferred_element_type=F32).astype(BF)
    outgoing = outgoing.reshape(64, 2, 2048)

    vmem = pl.BlockSpec(memory_space=pltpu.VMEM)
    hbm = pl.BlockSpec(memory_space=pl.ANY)
    mixer_out, back = pl.pallas_call(
        body,
        out_shape=(
            jax.ShapeDtypeStruct((64, 2048), BF),
            jax.ShapeDtypeStruct((64, 2, 2048), BF),
        ),
        in_specs=[vmem] * 3 + [hbm] * 4,
        out_specs=(vmem, vmem),
        scratch_shapes=[
            pltpu.VMEM((8, 2, 4, 256, 128), BF),
            pltpu.VMEM((2, 4, 32, 2, 2048), BF),
            pltpu.VMEM((256, 2048), BF),
            pltpu.VMEM((256, 896), BF),
            pltpu.VMEM((3, 4, 64, 2048), BF),
            pltpu.VMEM((3, 8, 32, 2048), BF),
            pltpu.VMEM((2, 32, 2, 2048), BF),
            pltpu.VMEM((256, 256), BF),
            pltpu.VMEM((4, 256, 1), F32),
            pltpu.VMEM((4, 256, 128), F32),
            pltpu.VMEM((2048, 896), BF),
            pltpu.VMEM((2048, 896), BF),
            pltpu.VMEM((896, 2048), BF),
            pltpu.VMEM((256, 2048), BF),
            pltpu.SemaphoreType.DMA((64,)),
            pltpu.SemaphoreType.DMA((64,)),
            pltpu.SemaphoreType.DMA((4,)),
        ],
        compiler_params=pltpu.CompilerParams(
            collective_id=0, has_side_effects=True, vmem_limit_bytes=60 << 20
        ),
        name="fused",
    )(
        rot_q,
        joined,
        outgoing,
        gate_weight[0],
        up_weight[0],
        down_weight[0],
        out_weight,
    )
    copies = jnp.dot(pick_hot, back.reshape(128, 2048), preferred_element_type=F32)
    weighted = route_weight[..., None] * copies.reshape(32, 2, 2048)
    mixed = jnp.sum(weighted, axis=1).astype(BF)
    return (mixer_out, mixed)


def solution(mesh):
    placed = (
        P("ep", "tp"),
        P("ep", "tp"),
        P("ep", "tp"),
        P(),
        P(),
        P("tp", None),
        P(("ep", "tp"), None),
        P(),
        P(("ep", "tp"), None),
        P(("ep", "tp"), None),
        P("ep", None, "tp"),
        P("ep", None, "tp"),
        P("ep", "tp", None),
    )
    return jax.shard_map(
        local,
        mesh=mesh,
        in_specs=placed,
        out_specs=(P(("ep", "tp"), None), P(("ep", "tp"), None)),
        check_vma=False,
    )
```

```python
import jax
import jax.numpy as jnp
import numpy as np
from jax import lax
from jax.experimental import pallas as pl
from jax.experimental.pallas import tpu as pltpu
from jax.sharding import PartitionSpec as P

EPS = 1e-06
THETA = 10000.0

NZ, NX = 8, 4
PLANES = (0, 7, 1, 4, 6, 2, 5, 3)
BF = jnp.bfloat16
F32 = jnp.float32
MESH = pl.DeviceIdType.MESH
RIGHT, OPP, LEFT = 1, 2, 3
F0, F1, D0, D1, E0, E1, S0, S1 = range(8)


def body(
    queries_hbm,
    keys_hbm,
    values_hbm,
    tokens_hbm,
    gate_hbm,
    up_hbm,
    down_hbm,
    ow_hbm,
    q_gain,
    k_gain,
    ffn_gain,
    freqs,
    route,
    weight,
    mix_ref,
    mixed_ref,
    kv,
    xs,
    xm,
    hid,
    part,
    rsb,
    ret,
    back_ref,
    outg_ref,
    picks,
    att,
    q_ref,
    m_s,
    acc,
    gate_v,
    up_v,
    down_v,
    ow_v,
    queries,
    keys,
    values,
    tokens,
    ssem,
    rsem,
    lsem,
):
    e = lax.axis_index("ep")
    t = lax.axis_index("tp")
    z, x, c = e // 8, lax.rem(e // 2, NX), lax.rem(e, 2)

    def dev(dz, dx, dc, dt=0):
        zz = lax.rem(z + (dz + NZ), NZ)
        xx = lax.rem(x + (dx + NX), NX)
        cc = c if dc == 0 else 1 - c
        tt = t if dt == 0 else lax.rem(t + (dt + 4), 4)
        return (zz * 8 + xx * 2 + cc, tt)

    used = [0]

    def sems():
        used[0] += 1
        return used[0] - 1

    def copy(src, dst, device, i=None):
        i = sems() if i is None else i
        return pltpu.make_async_remote_copy(
            src_ref=src,
            dst_ref=dst,
            send_sem=ssem.at[i],
            recv_sem=rsem.at[i],
            device_id=device,
            device_id_type=MESH,
        )

    up_dev, down_dev, partner = dev(1, 0, 0), dev(-1, 0, 0), dev(0, 0, 1)
    near, far = dev(0, 1, 0), dev(0, -1, 0)
    top, low = pl.ds(0, 128), pl.ds(128, 128)
    hop_up = [copy(kv.at[(8 - i) % 8, 0, 0], kv.at[7 - i, 0, 0], up_dev) for i in range(3)]
    hop_down = [copy(kv.at[i, 0, 0], kv.at[i + 1, 0, 0], down_dev) for i in range(3)]
    hop_up.append(copy(kv.at[5, 0, 0, top], kv.at[4, 0, 0, top], up_dev))
    hop_down.append(copy(kv.at[3, 0, 0, low], kv.at[4, 0, 0, low], down_dev))
    x_near = [copy(kv.at[d, 0, 0], kv.at[d, 0, 3], near) for d in range(NZ)]
    x_far = [copy(kv.at[d, 0, 0], kv.at[d, 0, 1], far) for d in range(NZ)]
    x_near2 = {d: copy(kv.at[d, 0, 3, top], kv.at[d, 0, 2, top], near) for d in range(1, NZ)}
    x_far2 = {d: copy(kv.at[d, 0, 1, low], kv.at[d, 0, 2, low], far) for d in range(1, NZ)}
    across = [copy(kv.at[d, 0], kv.at[d, 1], partner) for d in range(NZ)]
    x_two = copy(kv.at[0, 0, 0], kv.at[0, 0, 2], dev(0, 2, 0))

    spots = [
        (p, dx, dc) for p in range(NZ) for dx in range(NX) for dc in range(2)
    ]
    dsp_i, ret_i = [sems(), sems()], [sems(), sems()]
    dispatch, returns = [[], []], [[], []]
    for k, (p, dx, dc) in enumerate(spots):
        if k == 0:
            continue
        ch, j = k // 32, k % 32
        dz = PLANES[p]
        dispatch[ch].append(copy(outg_ref.at[k], xs.at[ch, 0, j], dev(-dz, -dx, dc), dsp_i[ch]))
        returns[ch].append(copy(ret.at[ch, j], back_ref.at[k], dev(dz, dx, dc), ret_i[ch]))

    def dispatch_all(ch):
        view = xs.at[ch, 0, pl.ds(1, 31)] if ch == 0 else xs.at[ch, 0]
        return copy(view, view, partner, dsp_i[ch])

    def return_all(ch):
        view = back_ref.at[pl.ds(1, 31)] if ch == 0 else back_ref.at[pl.ds(32, 32)]
        return copy(view, view, partner, ret_i[ch])

    right, left = dev(0, 0, 0, 1), dev(0, 0, 0, -1)
    lo, hi = pl.ds(0, 16), pl.ds(16, 16)
    ag = []
    for ch in range(2):
        ag.append(
            (
                copy(xs.at[ch, 0, lo], xs.at[ch, LEFT, lo], right),
                copy(xs.at[ch, 0, hi], xs.at[ch, RIGHT, hi], left),
                copy(xs.at[ch, 0, hi], xs.at[ch, LEFT, hi], right),
                copy(xs.at[ch, 0, lo], xs.at[ch, RIGHT, lo], left),
                copy(xs.at[ch, LEFT, lo], xs.at[ch, OPP, lo], right),
                copy(xs.at[ch, RIGHT, hi], xs.at[ch, OPP, hi], left),
            )
        )
    lo, hi = pl.ds(0, 32), pl.ds(32, 32)
    rs = []
    for i in range(3):
        pi, bi = part.at[i], rsb.at[i]
        rs.append(
            (
                copy(pi.at[OPP, lo], bi.at[F0], right),
                copy(pi.at[OPP, hi], bi.at[F1], left),
                copy(pi.at[RIGHT, hi], bi.at[D1], right),
                copy(pi.at[LEFT, lo], bi.at[D0], left),
                copy(bi.at[S0], bi.at[E0], right),
                copy(bi.at[S1], bi.at[E1], left),
            )
        )

    loads = [
        pltpu.make_async_copy(src, dst, lsem.at[i])
        for i, (src, dst) in enumerate(
            [
                (keys_hbm, keys),
                (values_hbm, values),
                (tokens_hbm, tokens),
                (queries_hbm, queries),
                (gate_hbm, gate_v),
                (up_hbm, up_v),
                (down_hbm, down_v),
                (ow_hbm, ow_v),
            ]
        )
    ]

    def gather_first(ch):
        dispatch_all(ch).wait_recv()
        for one in ag[ch][:4]:
            one.start()

    def gather_second(ch):
        ag[ch][0].wait_recv()
        ag[ch][4].start()
        ag[ch][1].wait_recv()
        ag[ch][5].start()

    def reduce_first(i):
        for one in rs[i][:4]:
            one.start()

    def reduce_middle(i, side):
        copied, slot, other, half, sent, way = (
            (0, F0, RIGHT, 0, S0, 4),
            (1, F1, LEFT, 32, S1, 5),
        )[side]
        rs[i][copied].wait_recv()
        for r in range(2):
            rows = pl.ds(16 * r, 16)
            own = part[i, other, pl.ds(half + 16 * r, 16)].astype(F32)
            rsb[i, sent, rows] = (rsb[i, slot, rows].astype(F32) + own).astype(BF)
        rs[i][way].start()

    def reduce_second(i):
        reduce_middle(i, 0)
        reduce_middle(i, 1)

    def reduce_last(i, store):
        for direct, passed, d, pe, half in ((3, 4, D0, E0, 0), (2, 5, D1, E1, 32)):
            rs[i][direct].wait_recv()
            rs[i][passed].wait_recv()
            for r in range(2):
                rows = pl.ds(16 * r, 16)
                total = (
                    part[i, 0, pl.ds(half + 16 * r, 16)].astype(F32)
                    + rsb[i, d, rows].astype(F32)
                    + rsb[i, pe, rows].astype(F32)
                ).astype(BF)
                store(half + 16 * r, total)

    def experts(ch, meanwhile):
        for n in (2, 3, 4, 5):
            ag[ch][n].wait_recv()
        if ch == 0:
            for one in loads[4:7]:
                one.wait()

        def relay(g, _):
            r, q = g // 4, lax.rem(g, 4)
            rows = xs[ch, r, pl.ds(q * 8, 8)].reshape(16, 2048)
            xm[pl.ds(pl.multiple_of(g * 16, 16), 16), :] = rows
            return 0

        lax.fori_loop(0, 16, relay, 0)

        def widen(n, _):
            cols = pl.ds(pl.multiple_of(n * 128, 128), 128)
            both = jnp.concatenate([gate_v[:, cols], up_v[:, cols]], axis=1)
            made = jnp.dot(xm[...], both, preferred_element_type=F32)
            gate, upper = made[:, :128], made[:, 128:]
            hid[:, cols] = (gate / (1.0 + jnp.exp(-gate)) * upper).astype(BF)
            return 0

        lax.fori_loop(0, 7, widen, 0, unroll=7)
        meanwhile()

        def narrow(n, _):
            cols = pl.ds(pl.multiple_of(n * 256, 256), 256)
            made = jnp.dot(hid[...], down_v[:, cols], preferred_element_type=F32).astype(BF)
            for r in range(4):
                part[ch, r, :, cols] = made[r * 64 : (r + 1) * 64]
            return 0

        lax.fori_loop(0, 8, narrow, 0, unroll=8)
        reduce_first(ch)

    def give_back(ch):
        def store(row, total):
            ret[ch, pl.ds(row // 2, 8)] = total.reshape(8, 2, 2048)

        reduce_last(ch, store)
        if ch == 0:
            back_ref[0] = ret[0, 0]
        for one in returns[ch]:
            one.start()

    barrier = pltpu.get_barrier_semaphore()
    for k, (p, dx, dc) in enumerate(spots):
        if k:
            pl.semaphore_signal(
                barrier, inc=1, device_id=dev(PLANES[p], dx, dc), device_id_type=MESH
            )
    for peer in (right, left):
        pl.semaphore_signal(barrier, inc=1, device_id=peer, device_id_type=MESH)
    for one in loads:
        one.start()

    lane = lax.broadcasted_iota(jnp.int32, (64, 128), 1)
    line = lax.broadcasted_iota(jnp.int32, (64, 128), 0)
    across_angle = line.astype(F32) * freqs[...]
    at_row = jnp.where(line[:8] < 4, line[:8], (line[:8] + t) & 3)
    down_angle = (at_row + e * 4).astype(F32) * freqs[...]
    even = (lane & 1) == 0
    by_row = (lane & 63) < 32
    first = lane < 64
    col_cos, col_sin = jnp.cos(across_angle), jnp.sin(across_angle)
    row_cos, row_sin = jnp.cos(down_angle), jnp.sin(down_angle)

    def turned(vals, gain, b):
        square = vals * vals
        one = jnp.sum(jnp.where(first, square, 0.0), axis=1, keepdims=True)
        two = jnp.sum(jnp.where(first, 0.0, square), axis=1, keepdims=True)
        mean = jnp.where(first, one, two) * (1.0 / 64)
        vals = vals * lax.rsqrt(mean + EPS) * gain
        swapped = jnp.where(even, pltpu.roll(vals, 127, 1), pltpu.roll(vals, 1, 1))
        cosine = jnp.where(by_row, row_cos[b : b + 1], col_cos)
        sine = jnp.where(by_row, row_sin[b : b + 1], col_sin)
        return vals * cosine + swapped * jnp.where(even, -sine, sine)

    loads[0].wait()
    loads[1].wait()
    gain = jnp.concatenate([k_gain[...], k_gain[...]], axis=1)
    for b in range(4):
        cols = pl.ds((b // 2) * 128, 128)
        half = slice((b % 2) * 64, (b % 2) * 64 + 64)
        key_rows = keys[:, cols].astype(F32).T[half]
        value_rows = values[:, cols].astype(F32).T[half]
        doubled = turned(jnp.concatenate([key_rows, key_rows], axis=1), gain, b)
        value_rows = jnp.concatenate([value_rows, value_rows], axis=1)
        kv[0, 0, 0, pl.ds(b * 64, 64), :] = jnp.where(first, doubled, value_rows).astype(BF)

    slot = lax.broadcasted_iota(jnp.int32, (128, 32), 0)
    spot, order = slot >> 1, (slot & 1).astype(F32)
    place = spot >> 3
    back_z = sum(jnp.where(place == p, dz, 0) for p, dz in enumerate(PLANES))
    target = (
        ((z + 8 - back_z) & 7) * 8
        + ((x + 4 - ((spot >> 1) & 3)) & 3) * 2
        + ((c + (spot & 1)) & 1)
    )
    named = [jnp.where(route[k : k + 1, :] == target, 1.0, 0.0) for k in range(2)]
    any_named = named[0] + named[1]
    rows_at = lax.broadcasted_iota(jnp.int32, (32, 32), 0)
    cols_at = lax.broadcasted_iota(jnp.int32, (32, 32), 1)
    before = jnp.where(rows_at < cols_at, 1.0, 0.0).astype(BF)
    rank = jnp.dot(any_named.astype(BF), before, preferred_element_type=F32)
    fits = jnp.where(rank == order, 1.0, 0.0)
    for k in range(2):
        picks[k] = (named[k] * fits).astype(BF)
    chosen = (any_named * fits).astype(BF)
    loads[2].wait()
    own = tokens[...].astype(F32)
    mean = jnp.mean(own * own, axis=1, keepdims=True)
    normed = (own * lax.rsqrt(mean + EPS) * ffn_gain[...]).astype(BF)
    for n in range(4):
        cols = slice(n * 512, n * 512 + 512)
        made = jnp.dot(chosen, normed[:, cols], preferred_element_type=F32)
        xm[0:128, cols] = made.astype(BF)

    def pack(g, _):
        rows = xm[pl.ds(pl.multiple_of(g * 16, 16), 16), :]
        outg_ref[pl.ds(g * 8, 8)] = rows.reshape(8, 2, 2048)
        return 0

    lax.fori_loop(0, 8, pack, 0)
    xs[0, 0, 0] = outg_ref[0]
    pl.semaphore_wait(barrier, 65)

    def send_rows(ch, planes):
        skip = 1 if ch == 0 else 0
        for p in planes:
            first_at = max(p * 8 - skip, 0)
            for one in dispatch[ch][first_at : p * 8 + 8 - skip]:
                one.start()

    def hops(d):
        if d:
            hop_up[d - 1].wait_recv()
            hop_down[d - 1].wait_recv()
        if d < 4:
            hop_up[d].start()
            hop_down[d].start()
        for at in {(8 - d) % 8, d}:
            x_near[at].start()
            x_far[at].start()

    def sides(d):
        for at in {(8 - d) % 8, d}:
            x_near[at].wait_recv()
            x_near2[at].start()
            x_far[at].wait_recv()
            x_far2[at].start()

    def cross(d):
        for at in {(8 - d) % 8, d}:
            x_near2[at].wait_recv()
            x_far2[at].wait_recv()
            across[at].start()

    hops(0)
    x_two.start()
    send_rows(0, range(4))
    loads[3].wait()
    gain = jnp.concatenate([q_gain[...], q_gain[...]], axis=1)
    for r in range(4):
        tokens_at = pl.ds(pl.multiple_of(lax.rem(t + r, 4) * 64, 64), 64)
        for pair in range(2):
            vals = queries[tokens_at, pair * 128 : pair * 128 + 128].astype(F32)
            done = turned(vals, gain, 4 + r).astype(BF).astype(F32) * 0.125
            rows = pl.ds(r * 256 + 2 * pair * 64, 64)
            q_ref[rows, :] = jnp.where(first, done, 0.0).astype(BF)
            rows = pl.ds(r * 256 + (2 * pair + 1) * 64, 64)
            q_ref[rows, :] = jnp.where(first, pltpu.roll(done, 64, 1), 0.0).astype(BF)
    m_s[...] = jnp.full_like(m_s, -1e30)
    acc[...] = jnp.zeros_like(acc)

    def at0():
        x_near[0].wait_recv()
        x_far[0].wait_recv()
        x_two.wait_recv()
        across[0].start()
        hops(1)
        send_rows(1, range(4))
        across[0].wait_recv()

    def in0():
        sides(1)
        gather_first(0)

    def at1():
        hops(2)
        cross(1)
        across[7].wait_recv()

    def in1():
        sides(2)
        hops(3)

    def at2():
        gather_second(0)
        gather_first(1)
        across[1].wait_recv()

    def in2():
        cross(2)
        sides(3)

    def at3():
        hops(4)
        experts(0, during0)
        across[6].wait_recv()

    def in3():
        cross(3)
        sides(4)

    def during0():
        gather_second(1)

    def during1():
        cross(4)
        reduce_second(0)

    def fold(high, total, scores, valued):
        above = jnp.maximum(high, jnp.max(scores, axis=1, keepdims=True))
        probs = jnp.exp(scores - above).astype(BF)
        made = jnp.dot(probs, valued, preferred_element_type=F32)
        return above, total * jnp.exp(high - above) + made

    def score(unit, keyed):
        return lax.dot_general(
            q_ref[pl.ds(pl.multiple_of(unit * 256, 256), 256), :],
            keyed,
            (((1,), (1,)), ((), ())),
            preferred_element_type=F32,
        )

    def with_ones(keyed):
        at = lax.broadcasted_iota(jnp.int32, keyed.shape, 1)
        return jnp.where(at == 0, jnp.ones_like(keyed), keyed)

    events = {0: at0, 1: at1, 2: at2, 3: at3}
    inside = {0: in0, 1: in1, 2: in2, 3: in3}

    def near_step(s, _):
        for at, event in events.items():
            pl.when(s == at)(event)
        odd = lax.rem(s, 2)
        dz = odd * (8 - (s + 1) // 2) + (1 - odd) * (s // 2)
        keyed = kv[dz].reshape(2048, 128)
        valued = with_ones(keyed)
        held = [(m_s[u], acc[u]) for u in range(4)]
        ahead = score(0, keyed)
        for u in range(4):
            now = ahead
            if u < 3:
                ahead = score(u + 1, keyed)
            m_s[u], acc[u] = fold(*held[u], now, valued)
            if u == 1:
                for at, event in inside.items():
                    pl.when(s == at)(event)
        return 0

    lax.fori_loop(0, 4, near_step, 0)

    experts(1, during1)
    for at in (2, 5, 3, 4):
        across[at].wait_recv()
    loads[7].wait()

    def between1():
        give_back(0)
        reduce_second(1)

    def between2():
        give_back(1)

    def far_step(s, _):
        for at, event in ((1, between1), (3, between2)):
            pl.when(s == at)(event)
        unit = lax.rem(2 + 3 * s + 3 * (s // 2) + 2 * (s // 3), 4)
        high, total = m_s[unit], acc[unit]
        blocks = [kv[dz].reshape(2048, 128) for dz in (2, 5, 3, 4)]
        ahead = score(unit, blocks[0])
        for i in range(4):
            now = ahead
            if i < 3:
                ahead = score(unit, blocks[i + 1])
            high, total = fold(high, total, now, with_ones(blocks[i]))
        scaled = (total / total[:, 0:1])[:, 64:].astype(BF)
        att[...] = jnp.concatenate([scaled[h * 64 : h * 64 + 64] for h in range(4)], axis=1)

        def project(n, _):
            cols = pl.ds(pl.multiple_of(n * 256, 256), 256)
            made = jnp.dot(att[...], ow_v[:, cols], preferred_element_type=F32)
            part[2, unit, :, cols] = made.astype(BF)
            return 0

        lax.fori_loop(0, 8, project, 0, unroll=8)

        @pl.when(s == 0)
        def _():
            rs[2][0].start()
            rs[2][1].start()

        @pl.when(s == 1)
        def _():
            rs[2][2].start()
            reduce_middle(2, 0)

        @pl.when(s == 2)
        def _():
            rs[2][3].start()
            reduce_middle(2, 1)

        return 0

    lax.fori_loop(0, 4, far_step, 0)

    def store_mix(row, total):
        mix_ref[pl.ds(row, 16), :] = total

    reduce_last(2, store_mix)
    for ch in range(2):
        return_all(ch).wait_recv()

    def unpack(g, _):
        rows = back_ref[pl.ds(g * 8, 8)].reshape(16, 2048)
        xm[pl.ds(pl.multiple_of(g * 16, 16), 16), :] = rows
        return 0

    lax.fori_loop(0, 8, unpack, 0)
    share = [
        jnp.sum(jnp.where(rows_at == cols_at, weight[k : k + 1, :], 0.0), axis=1, keepdims=True)
        for k in range(2)
    ]
    for n in range(4):
        cols = slice(n * 512, n * 512 + 512)
        came = [
            lax.dot_general(
                picks[k],
                xm[0:128, cols],
                (((0,), (0,)), ((), ())),
                preferred_element_type=F32,
            )
            for k in range(2)
        ]
        mixed_ref[:, cols] = (share[0] * came[0] + share[1] * came[1]).astype(BF)

    halves = [*x_near2.values(), *x_far2.values()]
    for one in [*hop_up, *hop_down, *x_near, *x_far, *halves, *across, x_two]:
        one.wait_send()
    for ch in range(2):
        dispatch_all(ch).wait_send()
        return_all(ch).wait_send()
        for one in ag[ch]:
            one.wait_send()
    for i in range(3):
        for one in rs[i]:
            one.wait_send()


def local(
    queries,
    keys,
    values,
    q_gain,
    k_gain,
    out_weight,
    tokens,
    ffn_gain,
    route,
    route_weight,
    gate_weight,
    up_weight,
    down_weight,
):
    pair = (np.arange(128) % 64) // 2
    freqs = np.power(THETA, -(pair % 16) / 16.0).astype(np.float32).reshape(1, 128)
    vmem = pl.BlockSpec(memory_space=pltpu.VMEM)
    hbm = pl.BlockSpec(memory_space=pl.ANY)
    return pl.pallas_call(
        body,
        out_shape=(
            jax.ShapeDtypeStruct((64, 2048), BF),
            jax.ShapeDtypeStruct((32, 2048), BF),
        ),
        in_specs=[hbm] * 8 + [vmem] * 6,
        out_specs=(vmem, vmem),
        scratch_shapes=[
            pltpu.VMEM((8, 2, 4, 256, 128), BF),
            pltpu.VMEM((2, 4, 32, 2, 2048), BF),
            pltpu.VMEM((256, 2048), BF),
            pltpu.VMEM((256, 896), BF),
            pltpu.VMEM((3, 4, 64, 2048), BF),
            pltpu.VMEM((3, 8, 32, 2048), BF),
            pltpu.VMEM((2, 32, 2, 2048), BF),
            pltpu.VMEM((64, 2, 2048), BF),
            pltpu.VMEM((64, 2, 2048), BF),
            pltpu.VMEM((2, 128, 32), BF),
            pltpu.VMEM((64, 256), BF),
            pltpu.VMEM((1024, 128), BF),
            pltpu.VMEM((4, 256, 1), F32),
            pltpu.VMEM((4, 256, 128), F32),
            pltpu.VMEM((2048, 896), BF),
            pltpu.VMEM((2048, 896), BF),
            pltpu.VMEM((896, 2048), BF),
            pltpu.VMEM((256, 2048), BF),
            pltpu.VMEM((256, 256), BF),
            pltpu.VMEM((64, 256), BF),
            pltpu.VMEM((64, 256), BF),
            pltpu.VMEM((32, 2048), BF),
            pltpu.SemaphoreType.DMA((96,)),
            pltpu.SemaphoreType.DMA((96,)),
            pltpu.SemaphoreType.DMA((8,)),
        ],
        compiler_params=pltpu.CompilerParams(
            collective_id=0, has_side_effects=True, vmem_limit_bytes=60 << 20
        ),
        name="fused",
    )(
        queries,
        keys.T,
        values.T,
        tokens,
        gate_weight[0],
        up_weight[0],
        down_weight[0],
        out_weight,
        q_gain.reshape(1, 64),
        k_gain.reshape(1, 64),
        ffn_gain.reshape(1, 2048),
        jnp.asarray(freqs),
        route.T,
        route_weight.T,
    )


def solution(mesh):
    placed = (
        P("ep", "tp"),
        P("ep", "tp"),
        P("ep", "tp"),
        P(),
        P(),
        P("tp", None),
        P(("ep", "tp"), None),
        P(),
        P(("ep", "tp"), None),
        P(("ep", "tp"), None),
        P("ep", None, "tp"),
        P("ep", None, "tp"),
        P("ep", "tp", None),
    )
    return jax.shard_map(
        local,
        mesh=mesh,
        in_specs=placed,
        out_specs=(P(("ep", "tp"), None), P(("ep", "tp"), None)),
        check_vma=False,
    )
```

```python
import jax
import jax.numpy as jnp
import numpy as np
from jax import lax
from jax.experimental import pallas as pl
from jax.experimental.pallas import tpu as pltpu
from jax.sharding import PartitionSpec as P

EPS = 1e-06
THETA = 10000.0

NZ, NX = 8, 4
PLANES = (0, 4, 1, 7, 5, 3, 6, 2)
BF = jnp.bfloat16
F32 = jnp.float32
MESH = pl.DeviceIdType.MESH
RIGHT, OPP, LEFT = 1, 2, 3
F0, F1, D0, D1, E0, E1, S0, S1 = range(8)


def body(
    queries_hbm,
    keys_hbm,
    values_hbm,
    tokens_hbm,
    gate_hbm,
    up_hbm,
    down_hbm,
    ow_hbm,
    q_gain,
    k_gain,
    ffn_gain,
    freqs,
    route,
    weight,
    mix_ref,
    mixed_ref,
    kv,
    xs,
    xm,
    hid,
    part,
    rsb,
    ret,
    back_ref,
    outg_ref,
    picks,
    att,
    q_ref,
    m_s,
    acc,
    gate_v,
    up_v,
    down_v,
    ow_v,
    queries,
    keys,
    values,
    tokens,
    ssem,
    rsem,
    lsem,
):
    e = lax.axis_index("ep")
    t = lax.axis_index("tp")
    z, x, c = e // 8, lax.rem(e // 2, NX), lax.rem(e, 2)

    def dev(dz, dx, dc, dt=0):
        zz = lax.rem(z + (dz + NZ), NZ)
        xx = lax.rem(x + (dx + NX), NX)
        cc = c if dc == 0 else 1 - c
        tt = t if dt == 0 else lax.rem(t + (dt + 4), 4)
        return (zz * 8 + xx * 2 + cc, tt)

    used = [0]

    def sems():
        used[0] += 1
        return used[0] - 1

    def copy(src, dst, device, i=None):
        i = sems() if i is None else i
        return pltpu.make_async_remote_copy(
            src_ref=src,
            dst_ref=dst,
            send_sem=ssem.at[i],
            recv_sem=rsem.at[i],
            device_id=device,
            device_id_type=MESH,
        )

    up_dev, down_dev, partner = dev(1, 0, 0), dev(-1, 0, 0), dev(0, 0, 1)
    near, far = dev(0, 1, 0), dev(0, -1, 0)
    top, low = pl.ds(0, 128), pl.ds(128, 128)
    hop_up = [copy(kv.at[(8 - i) % 8, 0, 0], kv.at[7 - i, 0, 0], up_dev) for i in range(3)]
    hop_down = [copy(kv.at[i, 0, 0], kv.at[i + 1, 0, 0], down_dev) for i in range(3)]
    hop_up.append(copy(kv.at[5, 0, 0, top], kv.at[4, 0, 0, top], up_dev))
    hop_down.append(copy(kv.at[3, 0, 0, low], kv.at[4, 0, 0, low], down_dev))
    x_near = [copy(kv.at[d, 0, 0], kv.at[d, 0, 3], near) for d in range(NZ)]
    x_far = [copy(kv.at[d, 0, 0], kv.at[d, 0, 1], far) for d in range(NZ)]
    x_near2 = {d: copy(kv.at[d, 0, 3, top], kv.at[d, 0, 2, top], near) for d in range(1, NZ)}
    x_far2 = {d: copy(kv.at[d, 0, 1, low], kv.at[d, 0, 2, low], far) for d in range(1, NZ)}
    across = [copy(kv.at[d, 0], kv.at[d, 1], partner) for d in range(NZ)]
    x_two = copy(kv.at[0, 0, 0], kv.at[0, 0, 2], dev(0, 2, 0))

    spots = [
        (p, dx, dc) for p in range(NZ) for dx in range(NX) for dc in range(2)
    ]
    dsp_i, ret_i = [sems(), sems()], [sems(), sems()]
    dispatch, returns = [[], []], [[], []]
    for k, (p, dx, dc) in enumerate(spots):
        if k == 0:
            continue
        ch, j = k // 32, k % 32
        dz = PLANES[p]
        dispatch[ch].append(copy(outg_ref.at[k], xs.at[ch, 0, j], dev(-dz, -dx, dc), dsp_i[ch]))
        returns[ch].append(copy(ret.at[ch, j], back_ref.at[k], dev(dz, dx, dc), ret_i[ch]))

    def dispatch_all(ch):
        view = xs.at[ch, 0, pl.ds(1, 31)] if ch == 0 else xs.at[ch, 0]
        return copy(view, view, partner, dsp_i[ch])

    def return_all(ch):
        view = back_ref.at[pl.ds(1, 31)] if ch == 0 else back_ref.at[pl.ds(32, 32)]
        return copy(view, view, partner, ret_i[ch])

    right, left = dev(0, 0, 0, 1), dev(0, 0, 0, -1)
    lo, hi = pl.ds(0, 16), pl.ds(16, 16)
    ag = []
    for ch in range(2):
        ag.append(
            (
                copy(xs.at[ch, 0, lo], xs.at[ch, LEFT, lo], right),
                copy(xs.at[ch, 0, hi], xs.at[ch, RIGHT, hi], left),
                copy(xs.at[ch, 0, hi], xs.at[ch, LEFT, hi], right),
                copy(xs.at[ch, 0, lo], xs.at[ch, RIGHT, lo], left),
                copy(xs.at[ch, LEFT, lo], xs.at[ch, OPP, lo], right),
                copy(xs.at[ch, RIGHT, hi], xs.at[ch, OPP, hi], left),
            )
        )
    lo, hi = pl.ds(0, 32), pl.ds(32, 32)
    rs = []
    for i in range(3):
        pi, bi = part.at[i], rsb.at[i]
        rs.append(
            (
                copy(pi.at[OPP, lo], bi.at[F0], right),
                copy(pi.at[OPP, hi], bi.at[F1], left),
                copy(pi.at[RIGHT, hi], bi.at[D1], right),
                copy(pi.at[LEFT, lo], bi.at[D0], left),
                copy(bi.at[S0], bi.at[E0], right),
                copy(bi.at[S1], bi.at[E1], left),
            )
        )

    loads = [
        pltpu.make_async_copy(src, dst, lsem.at[i])
        for i, (src, dst) in enumerate(
            [
                (keys_hbm, keys),
                (values_hbm, values),
                (tokens_hbm, tokens),
                (queries_hbm, queries),
                (gate_hbm, gate_v),
                (up_hbm, up_v),
                (down_hbm, down_v),
                (ow_hbm, ow_v),
            ]
        )
    ]

    def gather_first(ch):
        dispatch_all(ch).wait_recv()
        for one in ag[ch][:4]:
            one.start()

    def gather_second(ch):
        ag[ch][0].wait_recv()
        ag[ch][4].start()
        ag[ch][1].wait_recv()
        ag[ch][5].start()

    def reduce_first(i):
        for one in rs[i][:4]:
            one.start()

    def reduce_middle(i, side):
        copied, slot, other, half, sent, way = (
            (0, F0, RIGHT, 0, S0, 4),
            (1, F1, LEFT, 32, S1, 5),
        )[side]
        rs[i][copied].wait_recv()
        for r in range(2):
            rows = pl.ds(16 * r, 16)
            own = part[i, other, pl.ds(half + 16 * r, 16)].astype(F32)
            rsb[i, sent, rows] = (rsb[i, slot, rows].astype(F32) + own).astype(BF)
        rs[i][way].start()

    def reduce_second(i):
        reduce_middle(i, 0)
        reduce_middle(i, 1)

    def reduce_last(i, store):
        for direct, passed, d, pe, half in ((3, 4, D0, E0, 0), (2, 5, D1, E1, 32)):
            rs[i][direct].wait_recv()
            rs[i][passed].wait_recv()
            for r in range(2):
                rows = pl.ds(16 * r, 16)
                total = (
                    part[i, 0, pl.ds(half + 16 * r, 16)].astype(F32)
                    + rsb[i, d, rows].astype(F32)
                    + rsb[i, pe, rows].astype(F32)
                ).astype(BF)
                store(half + 16 * r, total)

    def experts(ch, meanwhile):
        for n in (2, 3, 4, 5):
            ag[ch][n].wait_recv()
        if ch == 0:
            for one in loads[4:7]:
                one.wait()

        def relay(g, _):
            r, q = g // 4, lax.rem(g, 4)
            rows = xs[ch, r, pl.ds(q * 8, 8)].reshape(16, 2048)
            xm[pl.ds(pl.multiple_of(g * 16, 16), 16), :] = rows
            return 0

        lax.fori_loop(0, 16, relay, 0)

        def widen(n, _):
            cols = pl.ds(pl.multiple_of(n * 128, 128), 128)
            both = jnp.concatenate([gate_v[:, cols], up_v[:, cols]], axis=1)
            made = jnp.dot(xm[...], both, preferred_element_type=F32)
            gate, upper = made[:, :128], made[:, 128:]
            hid[:, cols] = (gate / (1.0 + jnp.exp(-gate)) * upper).astype(BF)
            return 0

        lax.fori_loop(0, 7, widen, 0, unroll=7)
        meanwhile()

        def narrow(n, _):
            cols = pl.ds(pl.multiple_of(n * 256, 256), 256)
            made = jnp.dot(hid[...], down_v[:, cols], preferred_element_type=F32).astype(BF)
            for r in range(4):
                part[ch, r, :, cols] = made[r * 64 : (r + 1) * 64]
            return 0

        lax.fori_loop(0, 8, narrow, 0, unroll=8)
        reduce_first(ch)

    def give_back(ch):
        def store(row, total):
            ret[ch, pl.ds(row // 2, 8)] = total.reshape(8, 2, 2048)

        reduce_last(ch, store)
        if ch == 0:
            back_ref[0] = ret[0, 0]
        for one in returns[ch]:
            one.start()

    barrier = pltpu.get_barrier_semaphore()
    for k, (p, dx, dc) in enumerate(spots):
        if k:
            pl.semaphore_signal(
                barrier, inc=1, device_id=dev(PLANES[p], dx, dc), device_id_type=MESH
            )
    for peer in (right, left):
        pl.semaphore_signal(barrier, inc=1, device_id=peer, device_id_type=MESH)
    for one in loads:
        one.start()

    lane = lax.broadcasted_iota(jnp.int32, (64, 128), 1)
    line = lax.broadcasted_iota(jnp.int32, (64, 128), 0)
    across_angle = line.astype(F32) * freqs[...]
    at_row = jnp.where(line[:8] < 4, line[:8], (line[:8] + t) & 3)
    down_angle = (at_row + e * 4).astype(F32) * freqs[...]
    even = (lane & 1) == 0
    by_row = (lane & 63) < 32
    first = lane < 64
    col_cos, col_sin = jnp.cos(across_angle), jnp.sin(across_angle)
    row_cos, row_sin = jnp.cos(down_angle), jnp.sin(down_angle)

    def turned(vals, gain, b):
        square = vals * vals
        one = jnp.sum(jnp.where(first, square, 0.0), axis=1, keepdims=True)
        two = jnp.sum(jnp.where(first, 0.0, square), axis=1, keepdims=True)
        mean = jnp.where(first, one, two) * (1.0 / 64)
        vals = vals * lax.rsqrt(mean + EPS) * gain
        swapped = jnp.where(even, pltpu.roll(vals, 127, 1), pltpu.roll(vals, 1, 1))
        cosine = jnp.where(by_row, row_cos[b : b + 1], col_cos)
        sine = jnp.where(by_row, row_sin[b : b + 1], col_sin)
        return vals * cosine + swapped * jnp.where(even, -sine, sine)

    loads[0].wait()
    loads[1].wait()
    gain = jnp.concatenate([k_gain[...], k_gain[...]], axis=1)
    for b in range(4):
        cols = pl.ds((b // 2) * 128, 128)
        half = slice((b % 2) * 64, (b % 2) * 64 + 64)
        key_rows = keys[:, cols].astype(F32).T[half]
        value_rows = values[:, cols].astype(F32).T[half]
        doubled = turned(jnp.concatenate([key_rows, key_rows], axis=1), gain, b)
        value_rows = jnp.concatenate([value_rows, value_rows], axis=1)
        kv[0, 0, 0, pl.ds(b * 64, 64), :] = jnp.where(first, doubled, value_rows).astype(BF)

    slot = lax.broadcasted_iota(jnp.int32, (128, 32), 0)
    spot, order = slot >> 1, (slot & 1).astype(F32)
    place = spot >> 3
    back_z = sum(jnp.where(place == p, dz, 0) for p, dz in enumerate(PLANES))
    target = (
        ((z + 8 - back_z) & 7) * 8
        + ((x + 4 - ((spot >> 1) & 3)) & 3) * 2
        + ((c + (spot & 1)) & 1)
    )
    named = [jnp.where(route[k : k + 1, :] == target, 1.0, 0.0) for k in range(2)]
    any_named = named[0] + named[1]
    rows_at = lax.broadcasted_iota(jnp.int32, (32, 32), 0)
    cols_at = lax.broadcasted_iota(jnp.int32, (32, 32), 1)
    before = jnp.where(rows_at < cols_at, 1.0, 0.0).astype(BF)
    rank = jnp.dot(any_named.astype(BF), before, preferred_element_type=F32)
    fits = jnp.where(rank == order, 1.0, 0.0)
    for k in range(2):
        picks[k] = (named[k] * fits).astype(BF)
    chosen = (any_named * fits).astype(BF)
    loads[2].wait()
    own = tokens[...].astype(F32)
    mean = jnp.mean(own * own, axis=1, keepdims=True)
    normed = (own * lax.rsqrt(mean + EPS) * ffn_gain[...]).astype(BF)
    for n in range(4):
        cols = slice(n * 512, n * 512 + 512)
        made = jnp.dot(chosen, normed[:, cols], preferred_element_type=F32)
        xm[0:128, cols] = made.astype(BF)

    def pack(g, _):
        rows = xm[pl.ds(pl.multiple_of(g * 16, 16), 16), :]
        outg_ref[pl.ds(g * 8, 8)] = rows.reshape(8, 2, 2048)
        return 0

    lax.fori_loop(0, 8, pack, 0)
    xs[0, 0, 0] = outg_ref[0]
    pl.semaphore_wait(barrier, 65)

    def send_rows(ch, planes):
        skip = 1 if ch == 0 else 0
        for p in planes:
            first_at = max(p * 8 - skip, 0)
            for one in dispatch[ch][first_at : p * 8 + 8 - skip]:
                one.start()

    def hops(d):
        if d:
            hop_up[d - 1].wait_recv()
            hop_down[d - 1].wait_recv()
        if d < 4:
            hop_up[d].start()
            hop_down[d].start()
        for at in {(8 - d) % 8, d}:
            x_near[at].start()
            x_far[at].start()

    def sides(d):
        for at in {(8 - d) % 8, d}:
            x_near[at].wait_recv()
            x_near2[at].start()
            x_far[at].wait_recv()
            x_far2[at].start()

    def cross(d):
        for at in {(8 - d) % 8, d}:
            x_near2[at].wait_recv()
            x_far2[at].wait_recv()
            across[at].start()

    hops(0)
    x_two.start()
    send_rows(0, range(4))
    loads[3].wait()
    gain = jnp.concatenate([q_gain[...], q_gain[...]], axis=1)
    for r in range(4):
        tokens_at = pl.ds(pl.multiple_of(lax.rem(t + r, 4) * 64, 64), 64)
        for pair in range(2):
            vals = queries[tokens_at, pair * 128 : pair * 128 + 128].astype(F32)
            done = turned(vals, gain, 4 + r).astype(BF).astype(F32) * 0.125
            rows = pl.ds(r * 256 + 2 * pair * 64, 64)
            q_ref[rows, :] = jnp.where(first, done, 0.0).astype(BF)
            rows = pl.ds(r * 256 + (2 * pair + 1) * 64, 64)
            q_ref[rows, :] = jnp.where(first, pltpu.roll(done, 64, 1), 0.0).astype(BF)
    m_s[...] = jnp.full_like(m_s, -1e30)
    acc[...] = jnp.zeros_like(acc)

    def at0():
        x_near[0].wait_recv()
        x_far[0].wait_recv()
        x_two.wait_recv()
        across[0].start()
        hops(1)
        send_rows(1, range(4))
        across[0].wait_recv()

    def in0():
        gather_first(0)
        sides(1)

    def at1():
        hops(2)
        cross(1)
        across[7].wait_recv()
        gather_second(0)

    def in1():
        sides(2)
        hops(3)
        gather_first(1)

    def at2():
        across[1].wait_recv()

    def at3():
        hops(4)
        cross(2)
        sides(3)
        experts(0, during0)
        across[6].wait_recv()

    def in3():
        cross(3)
        sides(4)

    def during0():
        gather_second(1)

    def during1():
        cross(4)
        reduce_second(0)

    def fold(high, total, scores, valued):
        above = jnp.maximum(high, jnp.max(scores, axis=1, keepdims=True))
        probs = jnp.exp(scores - above).astype(BF)
        made = jnp.dot(probs, valued, preferred_element_type=F32)
        return above, total * jnp.exp(high - above) + made

    def score(unit, keyed):
        return lax.dot_general(
            q_ref[pl.ds(pl.multiple_of(unit * 256, 256), 256), :],
            keyed,
            (((1,), (1,)), ((), ())),
            preferred_element_type=F32,
        )

    def with_ones(keyed):
        at = lax.broadcasted_iota(jnp.int32, keyed.shape, 1)
        return jnp.where(at == 0, jnp.ones_like(keyed), keyed)

    events = {0: at0, 1: at1, 2: at2, 3: at3}
    inside = {0: in0, 1: in1, 3: in3}

    def near_step(s, _):
        for at, event in events.items():
            pl.when(s == at)(event)
        odd = lax.rem(s, 2)
        dz = odd * (8 - (s + 1) // 2) + (1 - odd) * (s // 2)
        keyed = kv[dz].reshape(2048, 128)
        valued = with_ones(keyed)
        held = [(m_s[u], acc[u]) for u in range(4)]
        ahead = score(0, keyed)
        for u in range(4):
            now = ahead
            if u < 3:
                ahead = score(u + 1, keyed)
            m_s[u], acc[u] = fold(*held[u], now, valued)
            if u == 1:
                for at, event in inside.items():
                    pl.when(s == at)(event)
        return 0

    lax.fori_loop(0, 4, near_step, 0)

    experts(1, during1)
    for at in (2, 5, 3):
        across[at].wait_recv()
    loads[7].wait()

    def mid1():
        reduce_second(1)
        rs[2][0].start()
        rs[2][1].start()

    def between3():
        give_back(1)

    def far_step(s, _):
        pl.when(s == 3)(between3)
        unit = lax.rem(2 + 3 * s + 3 * (s // 2) + 2 * (s // 3), 4)
        high, total = m_s[unit], acc[unit]

        def block(i):
            return kv[(2, 5, 3, 4)[i]].reshape(2048, 128)

        ahead = score(unit, block(0))
        for i in range(4):
            now = ahead
            if i < 3:
                ahead = score(unit, block(i + 1))
            high, total = fold(high, total, now, with_ones(block(i)))
            if i == 1:
                pl.when(s == 0)(across[4].wait_recv)
                pl.when(s == 1)(mid1)
        scaled = (total / total[:, 0:1])[:, 64:].astype(BF)
        att[...] = jnp.concatenate([scaled[h * 64 : h * 64 + 64] for h in range(4)], axis=1)

        def project(n, _):
            cols = pl.ds(pl.multiple_of(n * 256, 256), 256)
            made = jnp.dot(att[...], ow_v[:, cols], preferred_element_type=F32)
            part[2, unit, :, cols] = made.astype(BF)
            return 0

        lax.fori_loop(0, 8, project, 0, unroll=8)

        @pl.when(s == 0)
        def _():
            give_back(0)

        @pl.when(s == 1)
        def _():
            rs[2][2].start()

        @pl.when(s == 2)
        def _():
            rs[2][3].start()

        return 0

    lax.fori_loop(0, 4, far_step, 0)

    reduce_second(2)

    def store_mix(row, total):
        mix_ref[pl.ds(row, 16), :] = total

    reduce_last(2, store_mix)
    for ch in range(2):
        return_all(ch).wait_recv()

    def unpack(g, _):
        rows = back_ref[pl.ds(g * 8, 8)].reshape(16, 2048)
        xm[pl.ds(pl.multiple_of(g * 16, 16), 16), :] = rows
        return 0

    lax.fori_loop(0, 8, unpack, 0)
    share = [
        jnp.sum(jnp.where(rows_at == cols_at, weight[k : k + 1, :], 0.0), axis=1, keepdims=True)
        for k in range(2)
    ]
    for n in range(4):
        cols = slice(n * 512, n * 512 + 512)
        came = [
            lax.dot_general(
                picks[k],
                xm[0:128, cols],
                (((0,), (0,)), ((), ())),
                preferred_element_type=F32,
            )
            for k in range(2)
        ]
        mixed_ref[:, cols] = (share[0] * came[0] + share[1] * came[1]).astype(BF)

    halves = [*x_near2.values(), *x_far2.values()]
    for one in [*hop_up, *hop_down, *x_near, *x_far, *halves, *across, x_two]:
        one.wait_send()
    for ch in range(2):
        dispatch_all(ch).wait_send()
        return_all(ch).wait_send()
        for one in ag[ch]:
            one.wait_send()
    for i in range(3):
        for one in rs[i]:
            one.wait_send()


def write(one_ref, two_ref, one_out, two_out, sem):
    first = pltpu.make_async_copy(one_ref, one_out, sem.at[0])
    second = pltpu.make_async_copy(two_ref, two_out, sem.at[1])
    first.start()
    second.start()
    first.wait()
    second.wait()


def local(
    queries,
    keys,
    values,
    q_gain,
    k_gain,
    out_weight,
    tokens,
    ffn_gain,
    route,
    route_weight,
    gate_weight,
    up_weight,
    down_weight,
):
    pair = (np.arange(128) % 64) // 2
    freqs = np.power(THETA, -(pair % 16) / 16.0).astype(np.float32).reshape(1, 128)
    vmem = pl.BlockSpec(memory_space=pltpu.VMEM)
    hbm = pl.BlockSpec(memory_space=pl.ANY)
    made = pl.pallas_call(
        body,
        out_shape=(
            jax.ShapeDtypeStruct((64, 2048), BF),
            jax.ShapeDtypeStruct((32, 2048), BF),
        ),
        in_specs=[hbm] * 8 + [vmem] * 6,
        out_specs=(vmem, vmem),
        scratch_shapes=[
            pltpu.VMEM((8, 2, 4, 256, 128), BF),
            pltpu.VMEM((2, 4, 32, 2, 2048), BF),
            pltpu.VMEM((256, 2048), BF),
            pltpu.VMEM((256, 896), BF),
            pltpu.VMEM((3, 4, 64, 2048), BF),
            pltpu.VMEM((3, 8, 32, 2048), BF),
            pltpu.VMEM((2, 32, 2, 2048), BF),
            pltpu.VMEM((64, 2, 2048), BF),
            pltpu.VMEM((64, 2, 2048), BF),
            pltpu.VMEM((2, 128, 32), BF),
            pltpu.VMEM((64, 256), BF),
            pltpu.VMEM((1024, 128), BF),
            pltpu.VMEM((4, 256, 1), F32),
            pltpu.VMEM((4, 256, 128), F32),
            pltpu.VMEM((2048, 896), BF),
            pltpu.VMEM((2048, 896), BF),
            pltpu.VMEM((896, 2048), BF),
            pltpu.VMEM((256, 2048), BF),
            pltpu.VMEM((256, 256), BF),
            pltpu.VMEM((64, 256), BF),
            pltpu.VMEM((64, 256), BF),
            pltpu.VMEM((32, 2048), BF),
            pltpu.SemaphoreType.DMA((96,)),
            pltpu.SemaphoreType.DMA((96,)),
            pltpu.SemaphoreType.DMA((8,)),
        ],
        compiler_params=pltpu.CompilerParams(
            collective_id=0, has_side_effects=True, vmem_limit_bytes=60 << 20
        ),
        name="fused",
    )(
        queries,
        keys.T,
        values.T,
        tokens,
        gate_weight[0],
        up_weight[0],
        down_weight[0],
        out_weight,
        q_gain.reshape(1, 64),
        k_gain.reshape(1, 64),
        ffn_gain.reshape(1, 2048),
        jnp.asarray(freqs),
        route.T,
        route_weight.T,
    )
    return pl.pallas_call(
        write,
        out_shape=(
            jax.ShapeDtypeStruct((64, 2048), BF),
            jax.ShapeDtypeStruct((32, 2048), BF),
        ),
        in_specs=[vmem] * 2,
        out_specs=(hbm, hbm),
        scratch_shapes=[pltpu.SemaphoreType.DMA((2,))],
        name="write",
    )(*made)


def solution(mesh):
    placed = (
        P("ep", "tp"),
        P("ep", "tp"),
        P("ep", "tp"),
        P(),
        P(),
        P("tp", None),
        P(("ep", "tp"), None),
        P(),
        P(("ep", "tp"), None),
        P(("ep", "tp"), None),
        P("ep", None, "tp"),
        P("ep", None, "tp"),
        P("ep", "tp", None),
    )
    return jax.shard_map(
        local,
        mesh=mesh,
        in_specs=placed,
        out_specs=(P(("ep", "tp"), None), P(("ep", "tp"), None)),
        check_vma=False,
    )
```
